32 devices in a mesh: kv: 4 (over y, x), tp: 8 (over z, core).
Axes of the slice: x: 2, y: 2, z: 4, core: 2. Of those that a mesh axis runs over, the one named last changes fastest.
Arguments:
- tokens: bfloat16 [512, 2048], P('tp', 'kv'), may hold values from -16 to 16
- lengths: int32 [512], P('tp'), may hold values from 1 to 8192, 524288 in all
- query_weight: bfloat16 [2048, 1024], P(None, 'kv'), may hold values from -0.125 to 0.125
- key_weight: bfloat16 [2048, 1024], P(None, 'kv'), may hold values from -0.125 to 0.125
- value_weight: bfloat16 [2048, 1024], P(None, 'kv'), may hold values from -0.125 to 0.125
- gate_weight: bfloat16 [2048, 1024], P(None, 'kv'), may hold values from -0.125 to 0.125
- output_weight: bfloat16 [1024, 2048], P('kv'), may hold values from -0.1875 to 0.1875
- mixer_gain: float32 [2048], replicated, may hold values from 0.1 to 1.9
- group_gain: float32 [1024], P('kv'), may hold values from 0.1 to 1.9
- channel_gain: float32 [2048], P('kv'), may hold values from 0.1 to 1.9
- up_weight: bfloat16 [2048, 8192], P('kv', 'tp'), may hold values from -0.125 to 0.125
- down_weight: bfloat16 [8192, 2048], P('tp', 'kv'), may hold values from -0.0625 to 0.0625
- memory_state: float32 [512, 16, 64, 64], P('tp', 'kv'), may hold values from -0.6 to 0.6
Outputs:
- mixed: bfloat16 [512, 2048], P('tp', 'kv')
- new_state: float32 [512, 16, 64, 64], P('tp', 'kv')
The draws below stay inside these ranges and needn't reach their ends.
All inputs are finite; a program needn't handle non-finite values. No bound on the sum of `lengths` on one device may be relied on, other than what follows from the above.
Results may differ from the reference program's by a relative error of at most 0.012.
Values may be sent and summed in bfloat16 or wider, within the bound.
A program may use at most 64 MiB of HBM per device.

```python
import math
import jax
import jax.numpy as jnp
import numpy as np
from jax import lax

D = 2048
HEADS = 16
HEAD_DIM = 64
FF = 8192
BATCH = 512
RET_W = 1024


def draw_tokens(key, part):
    noise_key = jax.random.fold_in(key, 11)
    row_key = jax.random.fold_in(key, 12)
    column = jnp.exp(jnp.linspace(jnp.log(0.4), jnp.log(2.4), D)).astype(jnp.float32)
    noise = jax.random.normal(noise_key, (BATCH, D), jnp.float32)
    row_scale = jnp.exp(jax.random.uniform(row_key, (BATCH, 1), jnp.float32, jnp.log(0.5), jnp.log(2.0)))
    values = noise * row_scale * column[None, :]
    return jnp.clip(values, -16.0, 16.0).astype(jnp.bfloat16)


def block_scale(rng, extent, pieces, least, top_value):
    def one(axis_at, parts):
        steps = jax.random.uniform(jax.random.fold_in(jax.random.fold_in(rng, 6), axis_at), (parts,), jnp.float32, least / len(pieces), top_value / len(pieces))
        return jnp.repeat(jnp.exp(steps), extent[axis_at] // parts).reshape((-1,) + (1,) * (len(extent) - axis_at - 1))

    loudness = one(*pieces[0])
    for cut in pieces[1:]:
        loudness = loudness * one(*cut)
    return loudness


def length_profile(number_of, total, bound, slope):
    loads = [(1 << 20) // math.isqrt(grade ** slope) + 1 for grade in range(2, number_of + 1)]
    rest, given = total - bound - (number_of - 1), [1] * (number_of - 1)
    while rest > 0:
        free = [i for i in range(number_of - 1) if given[i] < bound]
        pool, budget = sum([loads[i] for i in free]), rest
        for i in free:
            extra = min(bound - given[i], max(1, budget * loads[i] // pool), rest)
            given[i] = given[i] + extra
            rest = rest - extra
    return np.array([bound] + given)


def uneven_parts(stream_key, number_of, total, most, skew):
    if number_of == 2:
        one = jax.random.randint(stream_key, (), max(1, total - most), min(most, total - 1) + 1)
        return jnp.stack([one, total - one])
    sizes = jnp.asarray(length_profile(number_of, total, most, skew), jnp.int32)
    pairs = (number_of - 1) // 2
    giver, taker = sizes[1:1 + 2 * pairs:2], sizes[2:2 + 2 * pairs:2]
    slack = jnp.minimum(giver - 1, most - taker)
    passed = jax.random.randint(jax.random.fold_in(stream_key, 1), (pairs,), 0, 1 << 20) % (slack + 1)
    sizes = sizes.at[1:1 + 2 * pairs:2].set(giver - passed).at[2:2 + 2 * pairs:2].set(taker + passed)
    return sizes[jax.random.permutation(jax.random.fold_in(stream_key, 2), number_of)]


def bell_draw(rng, shape, scale, limit, split=(), kind=jnp.bfloat16):
    values = scale * jax.random.normal(rng, shape, jnp.float32)
    if split:
        values = values * block_scale(rng, shape, split, -0.22, 0.18)
    return jnp.clip(values, -limit, limit).astype(kind)


def setup_inputs(seed: int = 0) -> dict:
    seeds = jax.random.split(jax.random.key(seed), 14)
    return {
        "tokens": draw_tokens(jax.random.fold_in(seeds[13], 71), 0),
        "lengths": uneven_parts(seeds[1], BATCH, BATCH * 1024, min(8192, BATCH * 256), 2).astype(jnp.int32),
        "query_weight": bell_draw(seeds[2], (D, RET_W), D ** -0.5, 0.125, ((1, 4),)),
        "key_weight": bell_draw(seeds[3], (D, RET_W), D ** -0.5, 0.125, ((1, 4),)),
        "value_weight": bell_draw(seeds[4], (D, RET_W), D ** -0.5, 0.125, ((1, 4),)),
        "gate_weight": bell_draw(seeds[5], (D, RET_W), D ** -0.5, 0.125, ((1, 4),)),
        "output_weight": bell_draw(seeds[6], (RET_W, D), RET_W ** -0.5, 0.1875, ((0, 4),)),
        "mixer_gain": jnp.clip(1.0 + 0.18 * jax.random.normal(seeds[7], (D,), jnp.float32), 0.1, 1.9),
        "group_gain": jnp.clip(1.0 + 0.18 * jax.random.normal(seeds[8], (RET_W,), jnp.float32), 0.1, 1.9),
        "channel_gain": jnp.clip(1.0 + 0.18 * jax.random.normal(seeds[9], (D,), jnp.float32), 0.1, 1.9),
        "up_weight": bell_draw(seeds[10], (D, FF), D ** -0.5, 0.125, ((0, 4), (1, 8))),
        "down_weight": bell_draw(seeds[11], (FF, D), FF ** -0.5, 0.0625, ((0, 8), (1, 4))),
        "memory_state": bell_draw(seeds[12], (BATCH, HEADS, HEAD_DIM, HEAD_DIM), 0.1, 0.6, ((0, 8), (1, 4)), jnp.float32),
    }


EPS = 1e-06
THETA = 10000.0

def rotate(vectors, position):
    breadth = vectors.shape[-1]
    middle = breadth // 2
    inverse = THETA ** (-jnp.arange(middle, dtype=jnp.float32) * 2.0 / breadth)
    angles = position.astype(jnp.float32)[:, None] * inverse[None, :]
    cosine = jnp.cos(angles)[:, None, :]
    sine_part = jnp.sin(angles)[:, None, :]
    former = vectors[..., :middle]
    latter = vectors[..., middle:]
    return jnp.concatenate([former * cosine - latter * sine_part, former * sine_part + latter * cosine], axis=-1)

def reference(tokens, lengths, query_weight, key_weight, value_weight, gate_weight, output_weight, mixer_gain, group_gain, channel_gain, up_weight, down_weight, memory_state):
    served = tokens.shape[0]
    widened = tokens.astype(jnp.float32)
    normed = (widened * lax.rsqrt(lax.optimization_barrier(jnp.mean(widened * widened, axis=1, keepdims=True)) + EPS) * mixer_gain.astype(jnp.float32)).astype(jnp.bfloat16)

    def project(weight):
        return jnp.dot(normed, weight, preferred_element_type=jnp.float32).reshape(served, HEADS, HEAD_DIM)
    queries = rotate(project(query_weight), lengths)
    keys_new = rotate(project(key_weight), lengths) * HEAD_DIM ** (-0.5)
    values_new = project(value_weight)
    gating = jnp.dot(normed, gate_weight, preferred_element_type=jnp.float32)
    head_ids = jnp.arange(HEADS).astype(jnp.float32)
    decays = 1.0 - 2.0 ** (-5.0 - 5.0 * head_ids / (HEADS - 1))
    new_state = decays[None, :, None, None] * memory_state + keys_new[:, :, :, None] * values_new[:, :, None, :]
    readout = jnp.einsum('bhkv,bhk->bhv', new_state, queries, precision=lax.Precision.HIGHEST)
    grouped = readout * lax.rsqrt(lax.optimization_barrier(jnp.mean(readout * readout, axis=-1, keepdims=True)) + EPS)
    grouped = grouped * group_gain.astype(jnp.float32).reshape(HEADS, HEAD_DIM)
    merged = (grouped.reshape(served, HEADS * HEAD_DIM) * jax.nn.silu(gating)).astype(jnp.bfloat16)
    mixed_part = jnp.dot(merged, output_weight, preferred_element_type=jnp.float32)
    after_mixer = (widened + mixed_part).astype(jnp.bfloat16)
    residual = after_mixer.astype(jnp.float32)
    factor = lax.rsqrt(lax.optimization_barrier(jnp.mean(residual * residual, axis=1)) + EPS)
    scaled = (residual * channel_gain.astype(jnp.float32)).astype(jnp.bfloat16)
    raised = jnp.dot(scaled, up_weight, preferred_element_type=jnp.float32) * factor[:, None]
    hidden = jnp.square(jax.nn.relu(raised)).astype(jnp.bfloat16)
    lowered = jnp.dot(hidden, down_weight, preferred_element_type=jnp.float32)
    return ((residual + lowered).astype(jnp.bfloat16), new_state)
```

```python
import functools

import jax
import jax.numpy as jnp
from jax import lax
from jax.experimental import pallas as pl
from jax.experimental.pallas import tpu as pltpu
from jax.sharding import PartitionSpec as P

HEADS = 16
HEAD_DIM = 64
EPS = 1e-06
THETA = 10000.0
CORES = 2
MESH = pl.DeviceIdType.MESH
BF = jnp.bfloat16
F32 = jnp.float32


def dot(a, b):
    return jnp.dot(a, b, preferred_element_type=F32)


def greet(groups):
    barrier = pltpu.get_barrier_semaphore()
    for device in groups:
        pl.semaphore_signal(barrier, inc=1, device_id=device, device_id_type=MESH)
    pl.semaphore_wait(barrier, len(groups))


def send(src, dst, send_sem, recv_sem, device):
    copy = pltpu.make_async_remote_copy(
        src_ref=src,
        dst_ref=dst,
        send_sem=send_sem,
        recv_sem=recv_sem,
        device_id=device,
        device_id_type=MESH,
    )
    copy.start()
    return copy


def head_kernel(
    parts, tok, gain, cosine, sine, wq, wk, wv, wg,
    q_out, k_out, v_out, g_out, rows, normed, own_sem, send_sem, recv_sem,
):
    kv = lax.axis_index("kv")
    peers = [{"kv": lax.rem(kv + d, parts)} for d in range(1, parts)]
    greet(peers)
    copies = [
        send(tok, rows.at[kv], send_sem.at[d], recv_sem.at[d], peer)
        for d, peer in enumerate(peers)
    ]
    own = pltpu.make_async_copy(tok, rows.at[kv], own_sem)
    own.start()
    own.wait()
    for copy in copies:
        copy.wait_recv()
    wide = tok.shape[1]
    total = jnp.zeros((tok.shape[0], 1), F32)
    for k in range(parts):
        x = rows[k].astype(F32)
        total = total + jnp.sum(x * x, axis=1, keepdims=True)
    scale = lax.rsqrt(total / (wide * parts) + EPS)
    for k in range(parts):
        x = rows[k].astype(F32)
        cols = pl.ds(k * wide, wide)
        normed[:, cols] = (x * scale * gain[:, cols]).astype(BF)
    n = normed[...]
    half = HEAD_DIM // 2
    width = wq.shape[1]

    def turn(x):
        lane = lax.broadcasted_iota(jnp.int32, x.shape, 1) % HEAD_DIM
        swapped = jnp.where(
            lane < half, pltpu.roll(x, width - half, 1), pltpu.roll(x, half, 1)
        )
        return x * cosine[...] + swapped * sine[...]

    if width % 128 == 0:
        q_out[...] = turn(dot(n, wq[...]))
        k_out[...] = turn(dot(n, wk[...])) * HEAD_DIM ** (-0.5)
    else:
        def turn_small(x):
            lane = lax.broadcasted_iota(jnp.int32, x.shape, 1) % HEAD_DIM
            swapped = jnp.where(
                lane < half,
                jnp.concatenate([x[:, half:], x[:, :half]], axis=1),
                jnp.concatenate([x[:, width - half:], x[:, : width - half]], axis=1),
            )
            return x * cosine[...] + swapped * sine[...]

        q_out[...] = turn_small(dot(n, wq[...]))
        k_out[...] = turn_small(dot(n, wk[...])) * HEAD_DIM ** (-0.5)
    v_out[...] = dot(n, wv[...])
    g_out[...] = dot(n, wg[...])
    for copy in copies:
        copy.wait_send()


def tail_kernel(
    parts, chips, merged, tok, ow, gain, up, down, out,
    s1, r1, x_all, s2, r2, hid, ps, pr, keep, s3, r3,
    s1_sem, r1_sem, ag_s, ag_r, fw_s, fw_r, s2_sem, r2_sem, hs_sem, hr_sem,
    ps_sem, pr_sem, s3_sem, r3_sem,
):
    kv = lax.axis_index("kv")
    tp = lax.axis_index("tp")
    z = tp // CORES
    c = tp % CORES
    peers = [{"kv": lax.rem(kv + d, parts)} for d in range(1, parts)]
    zpeers = [{"tp": lax.rem(z + d, chips) * CORES + c} for d in range(1, chips)]
    mate = {"tp": z * CORES + 1 - c}
    greet(peers + zpeers + [mate])
    served, wide = tok.shape
    group = CORES * served
    share = group // parts
    ff = up.shape[1]
    pending = []

    copies = []
    for d, peer in enumerate(peers):
        cols = pl.ds(pl.multiple_of(peer["kv"] * wide, wide), wide)
        s1[d] = dot(merged[...], ow[:, cols]).astype(BF)
        copies.append(send(s1.at[d], r1.at[d], s1_sem.at[d], r1_sem.at[d], peer))
    cols = pl.ds(pl.multiple_of(kv * wide, wide), wide)
    acc = dot(merged[...], ow[:, cols])
    for d, copy in enumerate(copies):
        copy.wait_recv()
        acc = acc + r1[d].astype(F32)
    pending += copies
    after = (tok[...].astype(F32) + acc).astype(BF)
    mine, other = pl.ds(0, served), pl.ds(served, served)
    x_all[0, mine] = after
    arrivals = [None] * chips
    for d, peer in enumerate(zpeers, 1):
        arrivals[chips - d] = send(
            x_all.at[0, mine], x_all.at[chips - d, mine],
            ag_s.at[d], ag_r.at[chips - d], peer,
        )
    forwards = [None] * chips
    forwards[0] = send(
        x_all.at[0, mine], x_all.at[0, other], fw_s.at[0], fw_r.at[0], mate
    )
    raised, gathered, paired, final = {}, {}, {}, {}

    def stage_a(s):
        if s:
            arrivals[s].wait_recv()
            forwards[s] = send(
                x_all.at[s, mine], x_all.at[s, other], fw_s.at[s], fw_r.at[s], mate
            )
        forwards[s].wait_recv()
        x = x_all[s].astype(F32)
        square = jnp.broadcast_to(jnp.sum(x * x, axis=1, keepdims=True), (group, 128))
        high = square.astype(BF)
        low = (square - high.astype(F32)).astype(BF)
        lane = lax.broadcasted_iota(jnp.int32, (group, 128), 1)
        tail = jnp.where(lane < 64, high.astype(F32), low.astype(F32))
        r = dot((x * gain[...]).astype(BF), up[...])
        for p in range(parts):
            part = slice(p * share, (p + 1) * share)
            s2[s, p, :, :ff] = r[part].astype(BF)
            s2[s, p, :, ff:] = tail[part].astype(BF)
        raised[s] = [
            send(
                s2.at[s, peer["kv"]], r2.at[s, d],
                s2_sem.at[s, d], r2_sem.at[s, d], peer,
            )
            for d, peer in enumerate(peers)
        ]

    def stage_b(s):
        acc = s2[s, kv].astype(F32)
        for d, copy in enumerate(raised[s]):
            copy.wait_recv()
            acc = acc + r2[s, d].astype(F32)
        total = jnp.sum(acc[:, ff:], axis=1, keepdims=True) * (1.0 / 64)
        factor = lax.rsqrt(total / (wide * parts) + EPS)
        hid[s, kv] = jnp.square(jnp.maximum(acc[:, :ff] * factor, 0.0)).astype(BF)
        gathered[s] = [
            send(
                hid.at[s, kv], hid.at[s, kv],
                hs_sem.at[s, d], hr_sem.at[s, d], peer,
            )
            for d, peer in enumerate(peers)
        ]

    def stage_c(s):
        for copy in gathered[s]:
            copy.wait_recv()
        h = jnp.concatenate([hid[s, p] for p in range(parts)], axis=0)
        lowered = dot(h, down[...])
        ps[s] = lowered[served:].astype(BF)
        paired[s] = send(ps.at[s], pr.at[s], ps_sem.at[s], pr_sem.at[s], mate)
        keep[s] = lowered[:served]

    def stage_d(s):
        paired[s].wait_recv()
        total = keep[s] + pr[s].astype(F32)
        if s == 0:
            keep[0] = total
        else:
            s3[s] = total.astype(BF)
            final[s] = send(
                s3.at[s], r3.at[chips - s],
                s3_sem.at[s], r3_sem.at[chips - s], zpeers[s - 1],
            )

    stages = (stage_a, stage_b, stage_c, stage_d)
    for t in range(chips + 3):
        for lag, stage in enumerate(stages):
            if 0 <= t - lag < chips:
                stage(t - lag)
    acc = keep[0]
    for s in range(1, chips):
        final[s].wait_recv()
        acc = acc + r3[chips - s].astype(F32)
    out[...] = (x_all[0, mine].astype(F32) + acc).astype(BF)
    for copy in pending + arrivals[1:] + forwards:
        copy.wait_send()
    for s in range(chips):
        for copy in raised[s] + gathered[s] + [paired[s]]:
            copy.wait_send()
        if s:
            final[s].wait_send()


VMEM = pl.BlockSpec(memory_space=pltpu.VMEM)
DMA = pltpu.SemaphoreType.DMA


def on_device(
    parts,
    chips,
    tokens,
    lengths,
    query_weight,
    key_weight,
    value_weight,
    gate_weight,
    output_weight,
    mixer_gain,
    group_gain,
    channel_gain,
    up_weight,
    down_weight,
    memory_state,
):
    served, wide = tokens.shape
    width = query_weight.shape[1]
    local_heads = width // HEAD_DIM
    half = HEAD_DIM // 2
    inverse = THETA ** (-jnp.arange(half, dtype=F32) * 2.0 / HEAD_DIM)
    angles = lengths.astype(F32)[:, None] * inverse[None, :]
    cosine, sine = jnp.cos(angles), jnp.sin(angles)
    cosine = jnp.concatenate([cosine, cosine] * local_heads, axis=1)
    sine = jnp.concatenate([-sine, sine] * local_heads, axis=1)
    projected = jax.ShapeDtypeStruct((served, width), F32)
    queries, keys_new, values_new, gating = pl.pallas_call(
        functools.partial(head_kernel, parts),
        out_shape=[projected] * 4,
        in_specs=[VMEM] * 8,
        out_specs=[VMEM] * 4,
        scratch_shapes=[
            pltpu.VMEM((parts, served, wide), BF),
            pltpu.VMEM((served, wide * parts), BF),
            DMA,
            DMA((parts - 1,)),
            DMA((parts - 1,)),
        ],
        compiler_params=pltpu.CompilerParams(collective_id=0, has_side_effects=True),
    )(
        tokens, mixer_gain[None, :], cosine, sine,
        query_weight, key_weight, value_weight, gate_weight,
    )
    queries = queries.reshape(served, local_heads, HEAD_DIM)
    keys_new = keys_new.reshape(served, local_heads, HEAD_DIM)
    values_new = values_new.reshape(served, local_heads, HEAD_DIM)
    head_ids = (lax.axis_index("kv") * local_heads + jnp.arange(local_heads)).astype(F32)
    decays = 1.0 - 2.0 ** (-5.0 - 5.0 * head_ids / (HEADS - 1))
    new_state = (
        decays[None, :, None, None] * memory_state
        + keys_new[:, :, :, None] * values_new[:, :, None, :]
    )
    readout = jnp.einsum("bhkv,bhk->bhv", new_state, queries, precision=lax.Precision.HIGHEST)
    grouped = readout * lax.rsqrt(jnp.mean(readout * readout, axis=-1, keepdims=True) + EPS)
    grouped = grouped * group_gain.reshape(local_heads, HEAD_DIM)
    merged = (grouped.reshape(served, width) * jax.nn.silu(gating)).astype(BF)

    ff = up_weight.shape[1]
    group = CORES * served
    share = group // parts
    pair = (chips, parts - 1)
    mixed = pl.pallas_call(
        functools.partial(tail_kernel, parts, chips),
        out_shape=jax.ShapeDtypeStruct((served, wide), BF),
        in_specs=[VMEM] * 6,
        out_specs=VMEM,
        scratch_shapes=[
            pltpu.VMEM((parts - 1, served, wide), BF),
            pltpu.VMEM((parts - 1, served, wide), BF),
            pltpu.VMEM((chips, group, wide), BF),
            pltpu.VMEM((chips, parts, share, ff + 128), BF),
            pltpu.VMEM((chips, parts - 1, share, ff + 128), BF),
            pltpu.VMEM((chips, parts, share, ff), BF),
            pltpu.VMEM((chips, served, wide), BF),
            pltpu.VMEM((chips, served, wide), BF),
            pltpu.VMEM((chips, served, wide), F32),
            pltpu.VMEM((chips, served, wide), BF),
            pltpu.VMEM((chips, served, wide), BF),
            DMA((parts - 1,)),
            DMA((parts - 1,)),
            DMA((chips,)),
            DMA((chips,)),
            DMA((chips,)),
            DMA((chips,)),
            DMA(pair),
            DMA(pair),
            DMA(pair),
            DMA(pair),
            DMA((chips,)),
            DMA((chips,)),
            DMA((chips,)),
            DMA((chips,)),
        ],
        compiler_params=pltpu.CompilerParams(collective_id=1, has_side_effects=True),
    )(merged, tokens, output_weight, channel_gain[None, :], up_weight, down_weight)
    return (mixed, new_state)


def solution(mesh):
    parts = mesh.shape["kv"]
    chips = mesh.shape["tp"] // CORES
    return jax.shard_map(
        functools.partial(on_device, parts, chips),
        mesh=mesh,
        in_specs=(
            P("tp", "kv"),
            P("tp"),
            P(None, "kv"),
            P(None, "kv"),
            P(None, "kv"),
            P(None, "kv"),
            P("kv", None),
            P(),
            P("kv"),
            P("kv"),
            P("kv", "tp"),
            P("tp", "kv"),
            P("tp", "kv", None, None),
        ),
        out_specs=(P("tp", "kv"), P("tp", "kv", None, None)),
        check_vma=False,
    )
```

```python
import functools

import jax
import jax.numpy as jnp
import numpy as np
from jax import lax
from jax.experimental import pallas as pl
from jax.experimental.pallas import tpu as pltpu
from jax.sharding import PartitionSpec as P

HEADS = 16
HEAD_DIM = 64
EPS = 1e-06
THETA = 10000.0
CORES = 2
MESH = pl.DeviceIdType.MESH
BF = jnp.bfloat16
F32 = jnp.float32


def dot(a, b):
    return jnp.dot(a, b, preferred_element_type=F32)


def greet(devices):
    barrier = pltpu.get_barrier_semaphore()
    for device in devices:
        pl.semaphore_signal(barrier, inc=1, device_id=device, device_id_type=MESH)


def greeted(devices):
    pl.semaphore_wait(pltpu.get_barrier_semaphore(), len(devices))


def send(src, dst, send_sem, recv_sem, device):
    copy = pltpu.make_async_remote_copy(
        src_ref=src,
        dst_ref=dst,
        send_sem=send_sem,
        recv_sem=recv_sem,
        device_id=device,
        device_id_type=MESH,
    )
    copy.start()
    return copy


def head_kernel(
    parts, tok, lengths, inverse, gain, wq, wk, wv, wg,
    q_out, k_out, v_out, g_out, rows, normed, weights, own_sem, w_sem, send_sem, recv_sem,
):
    kv = lax.axis_index("kv")
    peers = [{"kv": lax.rem(kv + d, parts)} for d in range(1, parts)]
    greet(peers)
    loads = [
        pltpu.make_async_copy(w, weights.at[i], w_sem.at[i])
        for i, w in enumerate((wq, wk, wv, wg))
    ]
    own = pltpu.make_async_copy(tok, rows.at[kv], own_sem)
    own.start()
    for load in loads:
        load.start()
    greeted(peers)
    copies = [
        send(tok, rows.at[kv], send_sem.at[d], recv_sem.at[d], peer)
        for d, peer in enumerate(peers)
    ]
    served, wide = tok.shape
    width = q_out.shape[1]
    half = HEAD_DIM // 2
    diagonal = lax.broadcasted_iota(jnp.int32, (served, served), 0) == (
        lax.broadcasted_iota(jnp.int32, (served, served), 1)
    )
    position = jnp.sum(
        jnp.where(diagonal, lengths[...].astype(F32), 0.0), axis=1, keepdims=True
    )
    angles = position * inverse[...]
    first = lax.broadcasted_iota(jnp.int32, (served, width), 1) % HEAD_DIM < half
    cosine = jnp.cos(angles)
    sine = jnp.where(first, -jnp.sin(angles), jnp.sin(angles))

    own.wait()
    for copy in copies:
        copy.wait_recv()
    total = jnp.zeros((served, 1), F32)
    for k in range(parts):
        x = rows[k].astype(F32)
        total = total + jnp.sum(x * x, axis=1, keepdims=True)
    scale = lax.rsqrt(total / (wide * parts) + EPS)
    for k in range(parts):
        x = rows[k].astype(F32)
        cols = pl.ds(k * wide, wide)
        normed[:, cols] = (x * scale * gain[:, cols]).astype(BF)
    n = normed[...]

    def turn(x):
        back = jnp.concatenate([x[:, half:], x[:, :half]], axis=1)
        ahead = jnp.concatenate([x[:, width - half :], x[:, : width - half]], axis=1)
        return x * cosine + jnp.where(first, back, ahead) * sine

    loads[0].wait()
    q_out[...] = turn(dot(n, weights[0]))
    loads[1].wait()
    k_out[...] = turn(dot(n, weights[1])) * HEAD_DIM ** (-0.5)
    loads[2].wait()
    v_out[...] = dot(n, weights[2])
    loads[3].wait()
    g_out[...] = dot(n, weights[3])
    for copy in copies:
        copy.wait_send()


def state_kernel(local, q, k, v, g, gain, state, new_state, merged, readout):
    step = pl.program_id(0)
    block = q.shape[0]
    first = lax.axis_index("kv") * local
    kt, q_t = k[...].T, q[...].T
    values = v[...]
    decays = []
    for h in range(local):
        head = jnp.full((1, HEAD_DIM), first + h, jnp.int32).astype(F32)
        decays.append(1.0 - jnp.exp2(-5.0 - 5.0 * head / (HEADS - 1)))
    rows = []
    for b in range(block):
        pieces = []
        for h in range(local):
            cut = slice(h * HEAD_DIM, (h + 1) * HEAD_DIM)
            new = decays[h] * state[b, h] + kt[cut, b : b + 1] * values[b : b + 1, cut]
            new_state[b, h] = new
            pieces.append(jnp.sum(new * q_t[cut, b : b + 1], axis=0, keepdims=True))
        rows.append(jnp.concatenate(pieces, axis=1))
    readout[pl.ds(pl.multiple_of(step * block, block), block)] = jnp.concatenate(rows, axis=0)

    @pl.when(step == pl.num_programs(0) - 1)
    def _():
        parts = []
        for h in range(local):
            x = readout[:, h * HEAD_DIM : (h + 1) * HEAD_DIM]
            parts.append(
                x * lax.rsqrt(jnp.mean(x * x, axis=1, keepdims=True) + EPS)
            )
        gate = g[...]
        merged[...] = (
            jnp.concatenate(parts, axis=1) * gain[...] * (gate * jax.nn.sigmoid(gate))
        ).astype(BF)


def tail_kernel(
    parts, chips, merged, tok, ow, gain, up_hbm, down_hbm, out,
    up, down, w_sem, s1, r1, x_all, s2, r2, hid, ps, pr, keep, s3, r3,
    s1_sem, r1_sem, ag_s, ag_r, fw_s, fw_r, s2_sem, r2_sem, hs_sem, hr_sem,
    ps_sem, pr_sem, s3_sem, r3_sem,
):
    kv = lax.axis_index("kv")
    tp = lax.axis_index("tp")
    z = tp // CORES
    c = tp % CORES
    peers = [{"kv": lax.rem(kv + d, parts)} for d in range(1, parts)]
    zpeers = [{"tp": lax.rem(z + d, chips) * CORES + c} for d in range(1, chips)]
    mate = {"tp": z * CORES + 1 - c}
    greet(peers + zpeers + [mate])
    loads = [
        pltpu.make_async_copy(up_hbm, up, w_sem.at[0]),
        pltpu.make_async_copy(down_hbm, down, w_sem.at[1]),
    ]
    for load in loads:
        load.start()
    served, wide = tok.shape
    group = CORES * served
    share = group // parts
    ff = up.shape[1]
    pending = []

    copies = []
    for d, peer in enumerate(peers):
        cols = pl.ds(pl.multiple_of(peer["kv"] * wide, wide), wide)
        s1[d] = dot(merged[...], ow[:, cols]).astype(BF)
        if d == 0:
            greeted(peers + zpeers + [mate])
        copies.append(send(s1.at[d], r1.at[d], s1_sem.at[d], r1_sem.at[d], peer))
    cols = pl.ds(pl.multiple_of(kv * wide, wide), wide)
    acc = dot(merged[...], ow[:, cols])
    for d, copy in enumerate(copies):
        copy.wait_recv()
        acc = acc + r1[d].astype(F32)
    pending += copies
    after = (tok[...].astype(F32) + acc).astype(BF)
    mine, other = pl.ds(0, served), pl.ds(served, served)
    x_all[0, mine] = after
    arrivals = [None] * chips
    for d, peer in enumerate(zpeers, 1):
        arrivals[chips - d] = send(
            x_all.at[0, mine], x_all.at[chips - d, mine],
            ag_s.at[d], ag_r.at[chips - d], peer,
        )
    forwards = [None] * chips
    forwards[0] = send(
        x_all.at[0, mine], x_all.at[0, other], fw_s.at[0], fw_r.at[0], mate
    )
    raised, gathered, paired, final = {}, {}, {}, {}

    def stage_a(s):
        if s:
            arrivals[s].wait_recv()
            forwards[s] = send(
                x_all.at[s, mine], x_all.at[s, other], fw_s.at[s], fw_r.at[s], mate
            )
        forwards[s].wait_recv()
        if s == 0:
            loads[0].wait()
        x = x_all[s].astype(F32)
        square = jnp.broadcast_to(jnp.sum(x * x, axis=1, keepdims=True), (group, 128))
        high = square.astype(BF)
        low = (square - high.astype(F32)).astype(BF)
        lane = lax.broadcasted_iota(jnp.int32, (group, 128), 1)
        tail = jnp.where(lane < 64, high.astype(F32), low.astype(F32))
        r = dot((x * gain[...]).astype(BF), up[...])
        for p in range(parts):
            part = slice(p * share, (p + 1) * share)
            s2[s, p, :, :ff] = r[part].astype(BF)
            s2[s, p, :, ff:] = tail[part].astype(BF)
        raised[s] = [
            send(
                s2.at[s, peer["kv"]], r2.at[s, d],
                s2_sem.at[s, d], r2_sem.at[s, d], peer,
            )
            for d, peer in enumerate(peers)
        ]

    def stage_b(s):
        acc = s2[s, kv].astype(F32)
        for d, copy in enumerate(raised[s]):
            copy.wait_recv()
            acc = acc + r2[s, d].astype(F32)
        total = jnp.sum(acc[:, ff:], axis=1, keepdims=True) * (1.0 / 64)
        factor = lax.rsqrt(total / (wide * parts) + EPS)
        hid[s, kv] = jnp.square(jnp.maximum(acc[:, :ff] * factor, 0.0)).astype(BF)
        gathered[s] = [
            send(
                hid.at[s, kv], hid.at[s, kv],
                hs_sem.at[s, d], hr_sem.at[s, d], peer,
            )
            for d, peer in enumerate(peers)
        ]

    def stage_c(s):
        for copy in gathered[s]:
            copy.wait_recv()
        if s == 0:
            loads[1].wait()
        h = jnp.concatenate([hid[s, p] for p in range(parts)], axis=0)
        lowered = dot(h, down[...])
        ps[s] = lowered[served:].astype(BF)
        paired[s] = send(ps.at[s], pr.at[s], ps_sem.at[s], pr_sem.at[s], mate)
        keep[s] = lowered[:served]

    def stage_d(s):
        paired[s].wait_recv()
        total = keep[s] + pr[s].astype(F32)
        if s == 0:
            keep[0] = total
        else:
            s3[s] = total.astype(BF)
            final[s] = send(
                s3.at[s], r3.at[chips - s],
                s3_sem.at[s], r3_sem.at[chips - s], zpeers[s - 1],
            )

    stages = (stage_a, stage_b, stage_c, stage_d)
    for t in range(chips + 3):
        for lag, stage in enumerate(stages):
            if 0 <= t - lag < chips:
                stage(t - lag)
    acc = keep[0]
    for s in range(1, chips):
        final[s].wait_recv()
        acc = acc + r3[chips - s].astype(F32)
    out[...] = (x_all[0, mine].astype(F32) + acc).astype(BF)
    for copy in pending + arrivals[1:] + forwards:
        copy.wait_send()
    for s in range(chips):
        for copy in raised[s] + gathered[s] + [paired[s]]:
            copy.wait_send()
        if s:
            final[s].wait_send()


VMEM = pl.BlockSpec(memory_space=pltpu.VMEM)
ANY = pl.BlockSpec(memory_space=pl.ANY)
DMA = pltpu.SemaphoreType.DMA


def on_device(
    parts,
    chips,
    tokens,
    lengths,
    query_weight,
    key_weight,
    value_weight,
    gate_weight,
    output_weight,
    mixer_gain,
    group_gain,
    channel_gain,
    up_weight,
    down_weight,
    memory_state,
):
    served, wide = tokens.shape
    width = query_weight.shape[1]
    local_heads = width // HEAD_DIM
    lane = np.arange(width) % (HEAD_DIM // 2)
    inverse = (THETA ** (-lane * 2.0 / HEAD_DIM)).astype(np.float32)[None, :]
    projected = jax.ShapeDtypeStruct((served, width), F32)
    queries, keys_new, values_new, gating = pl.pallas_call(
        functools.partial(head_kernel, parts),
        out_shape=[projected] * 4,
        in_specs=[VMEM] * 4 + [ANY] * 4,
        out_specs=[VMEM] * 4,
        scratch_shapes=[
            pltpu.VMEM((parts, served, wide), BF),
            pltpu.VMEM((served, wide * parts), BF),
            pltpu.VMEM((4,) + query_weight.shape, BF),
            DMA,
            DMA((4,)),
            DMA((parts - 1,)),
            DMA((parts - 1,)),
        ],
        compiler_params=pltpu.CompilerParams(collective_id=0, has_side_effects=True),
    )(
        tokens, lengths[None, :], jnp.asarray(inverse), mixer_gain[None, :],
        query_weight, key_weight, value_weight, gate_weight,
    )
    block = 8
    rows = pl.BlockSpec((block, width), lambda i: (i, 0))
    states = pl.BlockSpec((block,) + memory_state.shape[1:], lambda i: (i, 0, 0, 0))
    whole = pl.BlockSpec((served, width), lambda i: (0, 0))
    new_state, merged = pl.pallas_call(
        functools.partial(state_kernel, local_heads),
        grid=(served // block,),
        out_shape=[
            jax.ShapeDtypeStruct(memory_state.shape, F32),
            jax.ShapeDtypeStruct((served, width), BF),
        ],
        in_specs=[
            rows, rows, rows, whole,
            pl.BlockSpec((1, width), lambda i: (0, 0)), states,
        ],
        out_specs=[states, whole],
        scratch_shapes=[pltpu.VMEM((served, width), F32)],
        cost_estimate=pl.CostEstimate(
            flops=6 * memory_state.size, bytes_accessed=16 * memory_state.size, transcendentals=0
        ),
    )(queries, keys_new, values_new, gating, group_gain[None, :], memory_state)

    ff = up_weight.shape[1]
    group = CORES * served
    share = group // parts
    pair = (chips, parts - 1)
    mixed = pl.pallas_call(
        functools.partial(tail_kernel, parts, chips),
        out_shape=jax.ShapeDtypeStruct((served, wide), BF),
        in_specs=[VMEM] * 4 + [ANY] * 2,
        out_specs=VMEM,
        scratch_shapes=[
            pltpu.VMEM(up_weight.shape, BF),
            pltpu.VMEM(down_weight.shape, BF),
            DMA((2,)),
            pltpu.VMEM((parts - 1, served, wide), BF),
            pltpu.VMEM((parts - 1, served, wide), BF),
            pltpu.VMEM((chips, group, wide), BF),
            pltpu.VMEM((chips, parts, share, ff + 128), BF),
            pltpu.VMEM((chips, parts - 1, share, ff + 128), BF),
            pltpu.VMEM((chips, parts, share, ff), BF),
            pltpu.VMEM((chips, served, wide), BF),
            pltpu.VMEM((chips, served, wide), BF),
            pltpu.VMEM((chips, served, wide), F32),
            pltpu.VMEM((chips, served, wide), BF),
            pltpu.VMEM((chips, served, wide), BF),
            DMA((parts - 1,)),
            DMA((parts - 1,)),
            DMA((chips,)),
            DMA((chips,)),
            DMA((chips,)),
            DMA((chips,)),
            DMA(pair),
            DMA(pair),
            DMA(pair),
            DMA(pair),
            DMA((chips,)),
            DMA((chips,)),
            DMA((chips,)),
            DMA((chips,)),
        ],
        compiler_params=pltpu.CompilerParams(collective_id=1, has_side_effects=True),
    )(merged, tokens, output_weight, channel_gain[None, :], up_weight, down_weight)
    return (mixed, new_state)


def solution(mesh):
    parts = mesh.shape["kv"]
    chips = mesh.shape["tp"] // CORES
    return jax.shard_map(
        functools.partial(on_device, parts, chips),
        mesh=mesh,
        in_specs=(
            P("tp", "kv"),
            P("tp"),
            P(None, "kv"),
            P(None, "kv"),
            P(None, "kv"),
            P(None, "kv"),
            P("kv", None),
            P(),
            P("kv"),
            P("kv"),
            P("kv", "tp"),
            P("tp", "kv"),
            P("tp", "kv", None, None),
        ),
        out_specs=(P("tp", "kv"), P("tp", "kv", None, None)),
        check_vma=False,
    )
```

```python
import functools

import jax
import jax.numpy as jnp
import numpy as np
from jax import lax
from jax.experimental import pallas as pl
from jax.experimental.pallas import tpu as pltpu
from jax.sharding import PartitionSpec as P

HEADS = 16
HEAD_DIM = 64
EPS = 1e-06
THETA = 10000.0
CORES = 2
MESH = pl.DeviceIdType.MESH
BF = jnp.bfloat16
F32 = jnp.float32


def dot(a, b):
    return jnp.dot(a, b, preferred_element_type=F32)


def greet(devices):
    barrier = pltpu.get_barrier_semaphore()
    for device in devices:
        pl.semaphore_signal(barrier, inc=1, device_id=device, device_id_type=MESH)


def greeted(devices):
    pl.semaphore_wait(pltpu.get_barrier_semaphore(), len(devices))


def send(src, dst, send_sem, recv_sem, device):
    copy = pltpu.make_async_remote_copy(
        src_ref=src,
        dst_ref=dst,
        send_sem=send_sem,
        recv_sem=recv_sem,
        device_id=device,
        device_id_type=MESH,
    )
    copy.start()
    return copy


def head_kernel(
    parts, tok, lengths, inverse, gain, wq, wk, wv, wg,
    q_out, k_out, v_out, g_out, rows, normed, weights, own_sem, w_sem, send_sem, recv_sem,
):
    kv = lax.axis_index("kv")
    peers = [{"kv": lax.rem(kv + d, parts)} for d in range(1, parts)]
    greet(peers)
    loads = [
        pltpu.make_async_copy(w, weights.at[i], w_sem.at[i])
        for i, w in enumerate((wq, wk, wv, wg))
    ]
    own = pltpu.make_async_copy(tok, rows.at[kv], own_sem)
    own.start()
    for load in loads:
        load.start()
    greeted(peers)
    copies = [
        send(tok, rows.at[kv], send_sem.at[d], recv_sem.at[d], peer)
        for d, peer in enumerate(peers)
    ]
    served, wide = tok.shape
    width = q_out.shape[1]
    half = HEAD_DIM // 2
    diagonal = lax.broadcasted_iota(jnp.int32, (served, served), 0) == (
        lax.broadcasted_iota(jnp.int32, (served, served), 1)
    )
    position = jnp.sum(
        jnp.where(diagonal, lengths[...].astype(F32), 0.0), axis=1, keepdims=True
    )
    angles = position * inverse[...]
    first = lax.broadcasted_iota(jnp.int32, (served, width), 1) % HEAD_DIM < half
    cosine = jnp.cos(angles)
    sine = jnp.where(first, -jnp.sin(angles), jnp.sin(angles))

    own.wait()
    for copy in copies:
        copy.wait_recv()
    total = jnp.zeros((served, 1), F32)
    for k in range(parts):
        x = rows[k].astype(F32)
        total = total + jnp.sum(x * x, axis=1, keepdims=True)
    scale = lax.rsqrt(total / (wide * parts) + EPS)
    for k in range(parts):
        x = rows[k].astype(F32)
        cols = pl.ds(k * wide, wide)
        normed[:, cols] = (x * scale * gain[:, cols]).astype(BF)
    n = normed[...]

    def turn(x):
        back = jnp.concatenate([x[:, half:], x[:, :half]], axis=1)
        ahead = jnp.concatenate([x[:, width - half :], x[:, : width - half]], axis=1)
        return x * cosine + jnp.where(first, back, ahead) * sine

    loads[0].wait()
    q_out[...] = turn(dot(n, weights[0]))
    loads[1].wait()
    k_out[...] = turn(dot(n, weights[1])) * HEAD_DIM ** (-0.5)
    loads[2].wait()
    v_out[...] = dot(n, weights[2])
    loads[3].wait()
    g_out[...] = dot(n, weights[3])
    for copy in copies:
        copy.wait_send()


def state_kernel(local, q, k, v, g, gain, state, new_state, merged, readout, spread):
    step = pl.program_id(0)
    block = q.shape[0]
    first = lax.axis_index("kv") * local
    width = q.shape[1]
    both = jnp.concatenate([k[...], q[...]], axis=1)
    high = both.astype(BF).astype(F32)
    rest = both - high
    middle = rest.astype(BF).astype(F32)
    pieces = jnp.concatenate([high, middle, rest - middle], axis=0)
    shape = (3 * block, block * 128)
    pick = lax.broadcasted_iota(jnp.int32, shape, 0) % block == (
        lax.broadcasted_iota(jnp.int32, shape, 1) // 128
    )
    spread[...] = dot(pieces.T.astype(BF), jnp.where(pick, 1.0, 0.0).astype(BF))
    values = v[...]
    decays = []
    for h in range(local):
        head = jnp.full((1, HEAD_DIM), first + h, jnp.int32).astype(F32)
        decays.append(1.0 - jnp.exp2(-5.0 - 5.0 * head / (HEADS - 1)))
    rows = []
    for b in range(block):
        pieces = []
        for h in range(local):
            cut = slice(h * HEAD_DIM, (h + 1) * HEAD_DIM)
            lanes = slice(b * 128, b * 128 + HEAD_DIM)
            low = h * HEAD_DIM
            key = spread[low : low + HEAD_DIM, lanes]
            query = spread[width + low : width + low + HEAD_DIM, lanes]
            new = decays[h] * state[b, h] + key * values[b : b + 1, cut]
            new_state[b, h] = new
            pieces.append(jnp.sum(new * query, axis=0, keepdims=True))
        rows.append(jnp.concatenate(pieces, axis=1))
    readout[pl.ds(pl.multiple_of(step * block, block), block)] = jnp.concatenate(rows, axis=0)

    @pl.when(step == pl.num_programs(0) - 1)
    def _():
        parts = []
        for h in range(local):
            x = readout[:, h * HEAD_DIM : (h + 1) * HEAD_DIM]
            parts.append(
                x * lax.rsqrt(jnp.mean(x * x, axis=1, keepdims=True) + EPS)
            )
        gate = g[...]
        merged[...] = (
            jnp.concatenate(parts, axis=1) * gain[...] * (gate * jax.nn.sigmoid(gate))
        ).astype(BF)


def tail_kernel(
    parts, chips, merged, tok, ow, gain, up_hbm, down_hbm, out,
    up, down, w_sem, s1, r1, x_all, s2, r2, hid, ps, pr, keep, s3, r3,
    s1_sem, r1_sem, ag_s, ag_r, fw_s, fw_r, s2_sem, r2_sem, hs_sem, hr_sem,
    ps_sem, pr_sem, s3_sem, r3_sem,
):
    kv = lax.axis_index("kv")
    tp = lax.axis_index("tp")
    z = tp // CORES
    c = tp % CORES
    peers = [{"kv": lax.rem(kv + d, parts)} for d in range(1, parts)]

    def partner(d):
        at, bit = z, 1
        while bit <= d:
            if d // bit % 2:
                at = at + bit - 2 * bit * (z // bit % 2)
            bit *= 2
        return at

    zpeers = [{"tp": partner(d) * CORES + c} for d in range(1, chips)]
    mate = {"tp": z * CORES + 1 - c}
    greet(peers + zpeers + [mate])
    loads = [
        pltpu.make_async_copy(up_hbm, up, w_sem.at[0]),
        pltpu.make_async_copy(down_hbm, down, w_sem.at[1]),
    ]
    for load in loads:
        load.start()
    served, wide = tok.shape
    group = CORES * served
    share = group // parts
    ff = up.shape[1]
    pending = []

    copies = []
    for d, peer in enumerate(peers):
        cols = pl.ds(pl.multiple_of(peer["kv"] * wide, wide), wide)
        s1[d] = dot(merged[...], ow[:, cols]).astype(BF)
        if d == 0:
            greeted(peers + zpeers + [mate])
        copies.append(send(s1.at[d], r1.at[d], s1_sem.at[d], r1_sem.at[d], peer))
    cols = pl.ds(pl.multiple_of(kv * wide, wide), wide)
    acc = dot(merged[...], ow[:, cols])
    for d, copy in enumerate(copies):
        copy.wait_recv()
        acc = acc + r1[d].astype(F32)
    pending += copies
    after = (tok[...].astype(F32) + acc).astype(BF)
    mine, other = pl.ds(0, served), pl.ds(served, served)
    x_all[0, mine] = after
    arrivals = [None] * chips
    for d, peer in enumerate(zpeers, 1):
        arrivals[d] = send(
            x_all.at[0, mine], x_all.at[d, mine], ag_s.at[d], ag_r.at[d], peer
        )
    forwards = [None] * chips
    forwards[0] = send(
        x_all.at[0, mine], x_all.at[0, other], fw_s.at[0], fw_r.at[0], mate
    )
    raised, gathered, paired, final = {}, {}, {}, {}

    def stage_a(s):
        if s:
            arrivals[s].wait_recv()
            forwards[s] = send(
                x_all.at[s, mine], x_all.at[s, other], fw_s.at[s], fw_r.at[s], mate
            )
        forwards[s].wait_recv()
        if s == 0:
            loads[0].wait()
        x = x_all[s].astype(F32)
        square = jnp.broadcast_to(jnp.sum(x * x, axis=1, keepdims=True), (group, 128))
        high = square.astype(BF)
        low = (square - high.astype(F32)).astype(BF)
        lane = lax.broadcasted_iota(jnp.int32, (group, 128), 1)
        tail = jnp.where(lane < 64, high.astype(F32), low.astype(F32))
        r = dot((x * gain[...]).astype(BF), up[...])
        for p in range(parts):
            part = slice(p * share, (p + 1) * share)
            s2[s, p, :, :ff] = r[part].astype(BF)
            s2[s, p, :, ff:] = tail[part].astype(BF)
        raised[s] = [
            send(
                s2.at[s, peer["kv"]], r2.at[s, d],
                s2_sem.at[s, d], r2_sem.at[s, d], peer,
            )
            for d, peer in enumerate(peers)
        ]

    def stage_b(s):
        acc = s2[s, kv].astype(F32)
        for d, copy in enumerate(raised[s]):
            copy.wait_recv()
            acc = acc + r2[s, d].astype(F32)
        total = jnp.sum(acc[:, ff:], axis=1, keepdims=True) * (1.0 / 64)
        factor = lax.rsqrt(total / (wide * parts) + EPS)
        hid[s, kv] = jnp.square(jnp.maximum(acc[:, :ff] * factor, 0.0)).astype(BF)
        gathered[s] = [
            send(
                hid.at[s, kv], hid.at[s, kv],
                hs_sem.at[s, d], hr_sem.at[s, d], peer,
            )
            for d, peer in enumerate(peers)
        ]

    def stage_c(s):
        for copy in gathered[s]:
            copy.wait_recv()
        if s == order[0]:
            loads[1].wait()
        h = jnp.concatenate([hid[s, p] for p in range(parts)], axis=0)
        lowered = dot(h, down[...])
        ps[s] = lowered[served:].astype(BF)
        paired[s] = send(ps.at[s], pr.at[s], ps_sem.at[s], pr_sem.at[s], mate)
        keep[s] = lowered[:served]

    def stage_d(s):
        paired[s].wait_recv()
        total = keep[s] + pr[s].astype(F32)
        if s == 0:
            keep[0] = total
        else:
            s3[s] = total.astype(BF)
            final[s] = send(
                s3.at[s], r3.at[s], s3_sem.at[s], r3_sem.at[s], zpeers[s - 1]
            )

    order = [*range(1, chips), 0]
    for t in range(chips + 4):
        if t < chips:
            stage_a(t)
        for lag, stage in ((2, stage_b), (3, stage_c), (4, stage_d)):
            if 0 <= t - lag < chips:
                stage(order[t - lag])
    acc = keep[0]
    for s in range(1, chips):
        final[s].wait_recv()
        acc = acc + r3[s].astype(F32)
    out[...] = (x_all[0, mine].astype(F32) + acc).astype(BF)
    for copy in pending + arrivals[1:] + forwards:
        copy.wait_send()
    for s in range(chips):
        for copy in raised[s] + gathered[s] + [paired[s]]:
            copy.wait_send()
        if s:
            final[s].wait_send()


VMEM = pl.BlockSpec(memory_space=pltpu.VMEM)
ANY = pl.BlockSpec(memory_space=pl.ANY)
DMA = pltpu.SemaphoreType.DMA


def on_device(
    parts,
    chips,
    tokens,
    lengths,
    query_weight,
    key_weight,
    value_weight,
    gate_weight,
    output_weight,
    mixer_gain,
    group_gain,
    channel_gain,
    up_weight,
    down_weight,
    memory_state,
):
    served, wide = tokens.shape
    width = query_weight.shape[1]
    local_heads = width // HEAD_DIM
    lane = np.arange(width) % (HEAD_DIM // 2)
    inverse = (THETA ** (-lane * 2.0 / HEAD_DIM)).astype(np.float32)[None, :]
    projected = jax.ShapeDtypeStruct((served, width), F32)
    queries, keys_new, values_new, gating = pl.pallas_call(
        functools.partial(head_kernel, parts),
        out_shape=[projected] * 4,
        in_specs=[VMEM] * 4 + [ANY] * 4,
        out_specs=[VMEM] * 4,
        scratch_shapes=[
            pltpu.VMEM((parts, served, wide), BF),
            pltpu.VMEM((served, wide * parts), BF),
            pltpu.VMEM((4,) + query_weight.shape, BF),
            DMA,
            DMA((4,)),
            DMA((parts - 1,)),
            DMA((parts - 1,)),
        ],
        compiler_params=pltpu.CompilerParams(collective_id=0, has_side_effects=True),
    )(
        tokens, lengths[None, :], jnp.asarray(inverse), mixer_gain[None, :],
        query_weight, key_weight, value_weight, gate_weight,
    )
    block = 16
    rows = pl.BlockSpec((block, width), lambda i: (i, 0))
    states = pl.BlockSpec((block,) + memory_state.shape[1:], lambda i: (i, 0, 0, 0))
    whole = pl.BlockSpec((served, width), lambda i: (0, 0))
    new_state, merged = pl.pallas_call(
        functools.partial(state_kernel, local_heads),
        grid=(served // block,),
        out_shape=[
            jax.ShapeDtypeStruct(memory_state.shape, F32),
            jax.ShapeDtypeStruct((served, width), BF),
        ],
        in_specs=[
            rows, rows, rows, whole,
            pl.BlockSpec((1, width), lambda i: (0, 0)), states,
        ],
        out_specs=[states, whole],
        scratch_shapes=[
            pltpu.VMEM((served, width), F32),
            pltpu.VMEM((2 * width, block * 128), F32),
        ],
        cost_estimate=pl.CostEstimate(
            flops=6 * memory_state.size, bytes_accessed=16 * memory_state.size, transcendentals=0
        ),
    )(queries, keys_new, values_new, gating, group_gain[None, :], memory_state)

    ff = up_weight.shape[1]
    group = CORES * served
    share = group // parts
    pair = (chips, parts - 1)
    mixed = pl.pallas_call(
        functools.partial(tail_kernel, parts, chips),
        out_shape=jax.ShapeDtypeStruct((served, wide), BF),
        in_specs=[VMEM] * 4 + [ANY] * 2,
        out_specs=VMEM,
        scratch_shapes=[
            pltpu.VMEM(up_weight.shape, BF),
            pltpu.VMEM(down_weight.shape, BF),
            DMA((2,)),
            pltpu.VMEM((parts - 1, served, wide), BF),
            pltpu.VMEM((parts - 1, served, wide), BF),
            pltpu.VMEM((chips, group, wide), BF),
            pltpu.VMEM((chips, parts, share, ff + 128), BF),
            pltpu.VMEM((chips, parts - 1, share, ff + 128), BF),
            pltpu.VMEM((chips, parts, share, ff), BF),
            pltpu.VMEM((chips, served, wide), BF),
            pltpu.VMEM((chips, served, wide), BF),
            pltpu.VMEM((chips, served, wide), F32),
            pltpu.VMEM((chips, served, wide), BF),
            pltpu.VMEM((chips, served, wide), BF),
            DMA((parts - 1,)),
            DMA((parts - 1,)),
            DMA((chips,)),
            DMA((chips,)),
            DMA((chips,)),
            DMA((chips,)),
            DMA(pair),
            DMA(pair),
            DMA(pair),
            DMA(pair),
            DMA((chips,)),
            DMA((chips,)),
            DMA((chips,)),
            DMA((chips,)),
        ],
        compiler_params=pltpu.CompilerParams(collective_id=1, has_side_effects=True),
    )(merged, tokens, output_weight, channel_gain[None, :], up_weight, down_weight)
    return (mixed, new_state)


def solution(mesh):
    parts = mesh.shape["kv"]
    chips = mesh.shape["tp"] // CORES
    return jax.shard_map(
        functools.partial(on_device, parts, chips),
        mesh=mesh,
        in_specs=(
            P("tp", "kv"),
            P("tp"),
            P(None, "kv"),
            P(None, "kv"),
            P(None, "kv"),
            P(None, "kv"),
            P("kv", None),
            P(),
            P("kv"),
            P("kv"),
            P("kv", "tp"),
            P("tp", "kv"),
            P("tp", "kv", None, None),
        ),
        out_specs=(P("tp", "kv"), P("tp", "kv", None, None)),
        check_vma=False,
    )
```
